32 devices in a mesh: sp: 8 (over z, x), tp: 4 (over y, core).
Axes of the slice: x: 2, y: 2, z: 4, core: 2. Of those that a mesh axis runs over, the one named last changes fastest.
Arguments:
- queries: bfloat16 [2048, 1024], P('sp', 'tp'), may hold values from -200 to 200
- keys: bfloat16 [2048, 512], P('sp', 'tp'), may hold values from -8 to 8
- values: bfloat16 [2048, 512], P('sp', 'tp'), may hold values from -6 to 6
- forget_cum: float32 [2048, 8], P('sp', 'tp'), may hold values from -258 to 0, as said below
- out_weight: bfloat16 [1024, 2048], P('tp'), may hold values from -0.1875 to 0.1875
- residual: bfloat16 [2048, 2048], P(('sp', 'tp')), may hold values from -3 to 3
- norm_gain: float32 [2048], replicated, may hold values from 0.1 to 1.9
- expert_gate: bfloat16 [8, 2048, 3584], P('sp', None, 'tp'), may hold values from -0.125 to 0.125
- expert_up: bfloat16 [8, 2048, 3584], P('sp', None, 'tp'), may hold values from -0.125 to 0.125
- expert_down: bfloat16 [8, 3584, 2048], P('sp', 'tp'), may hold values from -0.09375 to 0.09375
- routes: int32 [2048, 2], P(('sp', 'tp')), may hold values from 0 to 7, all different within a row; in each aligned block of 64 rows (0 to 63, 64 to 127, ...) at most 24 rows name the same one
- route_weights: float32 [2048, 2], P(('sp', 'tp')), may hold values from 0.25 to 1
Outputs:
- layer_out: bfloat16 [2048, 2048], P(('sp', 'tp'))
The draws below stay inside these ranges and needn't reach their ends.
Inputs may be any that keep to these rules, and one draw needn't show every extreme that they name: `forget_cum`: each head's column never rises along the positions. `routes`: in the 64 rows of one device no expert is named more than 24 times, and in some devices' rows one expert exactly 24 times; the 2 entries of a row differ.
All inputs are finite; a program needn't handle non-finite values.
Results may differ from the reference program's by a relative error of at most 0.015.
Values may be sent and summed in bfloat16 or wider, within the bound.
No kernel may reach another device: no remote copies, remote signals or barrier semaphores. Data moves between devices by JAX's collectives and lax.ppermute only.
A program may use at most 128 MiB of HBM per device.

```python
import math
import jax
import jax.numpy as jnp
import numpy as np
from jax import lax

D = 2048
HEAD_COUNT = 8
KV_HEADS = 4
HEAD_DIM = 128
FF = 3584
TOP = 2
TOK_DEV = 256
SEQUENCE_LENGTH = 2048
ROWS = 64
EXPERTS = 8
CAP = 24
N_SP = 8
N_TP = 4


def drawn_pair(key):
    random_base_key = jax.random.fold_in(key, 11)
    key_rows = jnp.clip(jax.random.normal(jax.random.fold_in(random_base_key, 1), (SEQUENCE_LENGTH, KV_HEADS, HEAD_DIM), jnp.float32), -6.0, 6.0)
    query_rows = 2.5 * jnp.clip(jax.random.normal(jax.random.fold_in(random_base_key, 2), (SEQUENCE_LENGTH, HEAD_COUNT, HEAD_DIM), jnp.float32), -6.0, 6.0)
    return (query_rows.reshape(SEQUENCE_LENGTH, HEAD_COUNT * HEAD_DIM), key_rows.reshape(SEQUENCE_LENGTH, KV_HEADS * HEAD_DIM))


def draw_queries(key, part):
    return drawn_pair(key)[0].astype(jnp.bfloat16)


def draw_keys(key, part):
    return drawn_pair(key)[1].astype(jnp.bfloat16)


def draw_forget_cum(key, part):
    random_base_key = jax.random.fold_in(key, 23)
    fast_heads = jax.random.randint(jax.random.fold_in(random_base_key, 1), (HEAD_COUNT,), 0, 2) == 1
    fast_rate = jnp.exp(jax.random.uniform(jax.random.fold_in(random_base_key, 2), (HEAD_COUNT,), jnp.float32, jnp.log(0.01), jnp.log(1.0 / 30.0)))
    slow_rate = jnp.exp(jax.random.uniform(jax.random.fold_in(random_base_key, 3), (HEAD_COUNT,), jnp.float32, jnp.log(0.2), jnp.log(0.8))) / SEQUENCE_LENGTH
    decay_rate = jnp.where(fast_heads, fast_rate, slow_rate)
    block_count = SEQUENCE_LENGTH // TOK_DEV
    block_factor = jnp.exp(jax.random.uniform(jax.random.fold_in(random_base_key, 4), (block_count, 1), jnp.float32, jnp.log(0.5), jnp.log(2.0)))
    block_factor = jnp.repeat(block_factor, TOK_DEV, axis=0)
    rough_factor = jax.random.uniform(jax.random.fold_in(random_base_key, 5), (SEQUENCE_LENGTH, HEAD_COUNT), jnp.float32, 0.5, 1.5)
    gate_logarithm = -decay_rate[None, :] * block_factor * rough_factor
    spike_rows = jax.random.randint(jax.random.fold_in(random_base_key, 6), (2,), 0, SEQUENCE_LENGTH)
    spike_loss = jax.random.uniform(jax.random.fold_in(random_base_key, 7), (2, HEAD_COUNT), jnp.float32, 0.22, 0.5)
    gate_logarithm = gate_logarithm.at[spike_rows].add(-spike_loss)
    return jnp.cumsum(gate_logarithm, axis=0)


def block_levels(key, shape, split, low, largest):
    level = 1.0
    for dim, parts in split:
        draws = jax.random.uniform(jax.random.fold_in(jax.random.fold_in(key, 6), dim), (parts,), jnp.float32, low / len(split), largest / len(split))
        level = level * jnp.repeat(jnp.exp(draws), shape[dim] // parts).reshape((-1,) + (1,) * (len(shape) - 1 - dim))
    return level


def deal_out(own_key, own, number, rows, amount, top, bound, slope):
    ranking = jax.random.permutation(own_key, amount)
    heavy_load, usual = shares(amount, rows * top, bound, slope, True), shares(amount, rows * top, bound, slope, False)
    places = jnp.arange(amount)

    def named(lengths, rotation):
        used = int((lengths > 0).sum())
        fixed = max(1, used // 4)
        moved = fixed + (places - fixed + rotation * (used - fixed)) % max(1, amount - fixed)
        return jnp.zeros((amount,), jnp.int32).at[ranking[jnp.where(places < fixed, places, moved)]].set(jnp.asarray(lengths, jnp.int32))

    lengths = jnp.where(number % 4 == 0, named(heavy_load, number // 4), named(usual, number - number // 4 - 1))
    mixed = jax.random.permutation(jax.random.fold_in(own, 3), amount)
    source_of, taker = mixed[0:amount // 2 * 2:2], mixed[1:amount // 2 * 2:2]
    margin = jnp.minimum(lengths[source_of] - 1, bound - lengths[taker]) // 2
    margin = jnp.where((source_of == ranking[0]) | (taker == ranking[0]) | (lengths[taker] == 0), 0, jnp.maximum(margin, 0))
    moved = jax.random.randint(jax.random.fold_in(own, 4), (amount // 2,), 0, 1 << 20) % (margin + 1)
    lengths = lengths.at[source_of].add(-moved).at[taker].add(moved)
    items = jnp.searchsorted(jnp.cumsum(lengths), jnp.arange(rows * top), side="right").astype(jnp.int32)
    listing = items.reshape(top, rows).T
    listing = listing[jax.random.permutation(jax.random.fold_in(own, 1), rows)]
    rotation = jax.random.randint(jax.random.fold_in(own, 2), (rows, 1), 0, top)
    return jnp.take_along_axis(listing, (jnp.arange(top)[None, :] + rotation) % top, axis=1)


def shares(count, total, reach, skew, full):
    weights = [(1 << 20) // math.isqrt(standing ** skew) + 1 for standing in range(1, count + 1)]
    largest = reach if full else min(reach, max(-(-total // count), total * weights[0] // sum(weights)))
    least = 1 if total - largest >= count - 1 else 0
    counts, spare = [largest] + [least] * (count - 1), total - largest - least * (count - 1)
    while spare > 0:
        movable = [i for i in range(1, count) if counts[i] < largest] or [i for i in range(1, count) if counts[i] < reach]
        mass, left = sum([weights[i] for i in movable]), spare
        for i in movable:
            extra = min(reach - counts[i], max(1, left * weights[i] // mass), spare)
            counts[i] = counts[i] + extra
            spare = spare - extra
    return np.array(counts)


def noise(key, dims, spread, most, cuts=(), kind=jnp.bfloat16):
    level = block_levels(key, dims, cuts, -0.22, 0.18) if cuts else 1.0
    result = jax.random.normal(key, dims, jnp.float32) * spread * level
    return jnp.minimum(jnp.maximum(result, -most), most).astype(kind)


def setup_inputs(seed: int = 0) -> dict:
    key_list = jax.random.split(jax.random.key(seed), 13)
    queries = draw_queries(jax.random.fold_in(key_list[12], 71), 0)
    keys = draw_keys(jax.random.fold_in(key_list[12], 71), 0)
    values = noise(key_list[2], (SEQUENCE_LENGTH, KV_HEADS * HEAD_DIM), 1.0, 6.0, ((0, 8), (1, 4)))
    forget_cum = draw_forget_cum(jax.random.fold_in(key_list[12], 71), 0)
    out_weight = noise(key_list[4], (HEAD_COUNT * HEAD_DIM, D), (HEAD_COUNT * HEAD_DIM) ** -0.5, 0.1875, ((0, 4),))
    residual = noise(key_list[5], (SEQUENCE_LENGTH, D), 0.5, 3.0, ((0, 32),))
    norm_gain = jnp.clip(1.0 + 0.18 * jax.random.normal(key_list[6], (D,), jnp.float32), 0.1, 1.9)
    expert_gate = noise(key_list[7], (EXPERTS, D, FF), D ** -0.5, 0.125, ((0, 8), (2, 4)))
    expert_up = noise(key_list[8], (EXPERTS, D, FF), D ** -0.5, 0.125, ((0, 8), (2, 4)))
    expert_down = noise(key_list[9], (EXPERTS, FF, D), FF ** -0.5, 0.09375, ((0, 8), (1, 4)))
    routes_keys = jax.random.split(jax.random.fold_in(key_list[10], 1), SEQUENCE_LENGTH // ROWS)
    routes_turns = jax.random.permutation(jax.random.fold_in(key_list[10], 3), SEQUENCE_LENGTH // ROWS)
    routes = jax.vmap(lambda own, number: deal_out(jax.random.fold_in(key_list[10], 2), own, number, ROWS, EXPERTS, TOP, CAP, 2))(routes_keys, routes_turns).reshape((SEQUENCE_LENGTH, TOP))
    route_weights = jnp.clip(0.25 + 0.75 * jax.random.uniform(key_list[11], (SEQUENCE_LENGTH, TOP), jnp.float32) ** block_levels(key_list[11], (SEQUENCE_LENGTH, TOP), ((0, 32),), -0.2, 0.2), 0.25, 1.0)
    return {"queries": queries, "keys": keys, "values": values, "forget_cum": forget_cum, "out_weight": out_weight, "residual": residual, "norm_gain": norm_gain, "expert_gate": expert_gate, "expert_up": expert_up, "expert_down": expert_down, "routes": routes, "route_weights": route_weights}


def reference(queries, keys, values, forget_cum, out_weight, residual, norm_gain, expert_gate, expert_up, expert_down, routes, route_weights):
    group_size = HEAD_COUNT // KV_HEADS
    score_scale = HEAD_DIM ** (-0.5)
    block_len = math.gcd(SEQUENCE_LENGTH, 512)
    block_count = SEQUENCE_LENGTH // block_len
    query_blocks = queries.reshape(block_count, block_len, KV_HEADS, group_size, HEAD_DIM)
    cum_blocks = forget_cum.reshape(block_count, block_len, KV_HEADS, group_size)
    index_blocks = jnp.arange(SEQUENCE_LENGTH, dtype=jnp.int32).reshape(block_count, block_len)
    key_heads = keys.reshape(SEQUENCE_LENGTH, KV_HEADS, HEAD_DIM).astype(jnp.float32)
    value_heads = values.reshape(SEQUENCE_LENGTH, KV_HEADS, HEAD_DIM).astype(jnp.float32)
    key_bias = jnp.transpose(forget_cum.reshape(SEQUENCE_LENGTH, KV_HEADS, group_size), (1, 2, 0))
    key_index = jnp.arange(SEQUENCE_LENGTH, dtype=jnp.int32)

    def causal_attend(block_arguments):
        query_now, cum_now, index_now = block_arguments
        scores = jnp.einsum('tkgd,ukd->tkgu', query_now.astype(jnp.float32), key_heads) * score_scale
        scores = scores + cum_now[..., None] - key_bias[None]
        visible = key_index[None, :] <= index_now[:, None]
        scores = jnp.where(visible[:, None, None, :], scores, -jnp.inf)
        row_max = lax.optimization_barrier(jnp.max(scores, axis=-1, keepdims=True))
        weights_exp = jnp.exp(scores - row_max)
        denominator = lax.optimization_barrier(jnp.sum(weights_exp, axis=-1))
        probs = weights_exp.astype(jnp.bfloat16)
        weighted = jnp.einsum('tkgu,ukd->tkgd', probs.astype(jnp.float32), value_heads)
        return (weighted / denominator[..., None]).astype(jnp.bfloat16).reshape(block_len, HEAD_COUNT * HEAD_DIM)
    heads_out = lax.map(causal_attend, (query_blocks, cum_blocks, index_blocks)).reshape(SEQUENCE_LENGTH, HEAD_COUNT * HEAD_DIM)
    projected = jnp.dot(heads_out, out_weight, preferred_element_type=jnp.float32)
    after_mix = (residual.astype(jnp.float32) + projected).astype(jnp.bfloat16)
    after_wide = after_mix.astype(jnp.float32)
    normed = (after_wide * lax.rsqrt(lax.optimization_barrier(jnp.mean(after_wide * after_wide, axis=-1, keepdims=True)) + 1e-06) * norm_gain).astype(jnp.bfloat16)
    pair_count = SEQUENCE_LENGTH * TOP
    flat_routes = routes.reshape(pair_count)
    most_rows = N_SP * N_TP * CAP
    width_block = FF // N_TP

    def expert_step(state_now, expert):
        chosen = flat_routes == expert
        live_rows = jnp.sum(chosen.astype(jnp.int32))
        slot_pairs = jnp.nonzero(chosen, size=most_rows, fill_value=0)[0].astype(jnp.int32)
        live = jnp.arange(most_rows, dtype=jnp.int32) < live_rows
        inputs = normed[slot_pairs // TOP]
        gate_val = jnp.dot(inputs, expert_gate[expert], preferred_element_type=jnp.float32)
        up_val = jnp.dot(inputs, expert_up[expert], preferred_element_type=jnp.float32)
        hidden = (jax.nn.silu(gate_val) * up_val).astype(jnp.bfloat16)
        pieces = jnp.einsum('mbf,bfd->bmd', hidden.reshape(most_rows, N_TP, width_block).astype(jnp.float32), expert_down[expert].reshape(N_TP, width_block, D).astype(jnp.float32))
        expert_out = lax.optimization_barrier(jnp.sum(pieces.astype(jnp.bfloat16).astype(jnp.float32), axis=0)).astype(jnp.bfloat16).astype(jnp.float32)
        state_now = state_now.at[slot_pairs].add(jnp.where(live[:, None], expert_out, 0.0))
        return (state_now, None)
    pair_out, _ = lax.scan(expert_step, jnp.zeros((pair_count, D), jnp.float32), jnp.arange(EXPERTS, dtype=jnp.int32))
    routed = lax.optimization_barrier(jnp.sum(route_weights[..., None] * pair_out.reshape(SEQUENCE_LENGTH, TOP, D), axis=1))
    return (after_wide + routed).astype(jnp.bfloat16)
```

```python
import jax
import jax.numpy as jnp
from jax import lax
from jax.sharding import PartitionSpec as P

HEAD_DIM = 128


def wide_shards(
    queries,
    keys,
    values,
    forget_cum,
    out_weight,
    residual,
    norm_gain,
    expert_gate,
    expert_up,
    expert_down,
    routes,
    route_weights,
):
    tok_rows = queries.shape[0]
    heads_here = forget_cum.shape[1]
    kv_heads_here = keys.shape[1] // HEAD_DIM
    group_size = heads_here // kv_heads_here
    score_scale = HEAD_DIM ** (-0.5)
    query_heads = queries.reshape(tok_rows, kv_heads_here, group_size, HEAD_DIM)
    own_cum = forget_cum.reshape(tok_rows, kv_heads_here, group_size)
    query_index = lax.axis_index("sp") * tok_rows + jnp.arange(tok_rows, dtype=jnp.int32)
    last_query = lax.axis_index("sp") * tok_rows + tok_rows - 1
    all_cum = lax.all_gather(forget_cum, "sp", axis=0, tiled=True)

    def span_step(running, span_args):
        keys_now, values_now, cum_now, start_now = span_args
        key_span = keys_now.shape[0]

        def scored(running_in):
            running_max, denominator, weighted = running_in
            scores = (
                jnp.einsum(
                    "tkgd,ukd->tkgu", query_heads, keys_now, preferred_element_type=jnp.float32
                )
                * score_scale
            )
            scores = scores + own_cum[..., None] - cum_now[None]
            key_index = start_now + jnp.arange(key_span, dtype=jnp.int32)
            visible = key_index[None, :] <= query_index[:, None]
            scores = jnp.where(visible[:, None, None, :], scores, -jnp.inf)
            new_max = jnp.maximum(running_max, jnp.max(scores, axis=-1))
            weights_exp = jnp.exp(scores - new_max[..., None])
            rescale = jnp.exp(running_max - new_max)
            denominator = denominator * rescale + jnp.sum(weights_exp, axis=-1)
            weighted = weighted * rescale[..., None] + jnp.einsum(
                "tkgu,ukd->tkgd",
                weights_exp.astype(jnp.bfloat16),
                values_now,
                preferred_element_type=jnp.float32,
            )
            return (new_max, denominator, weighted)

        def skipped(running_in):
            return running_in

        return (lax.cond(start_now <= last_query, scored, skipped, running), None)

    start_state = (
        jnp.full((tok_rows, kv_heads_here, group_size), -1e30, jnp.float32),
        jnp.zeros((tok_rows, kv_heads_here, group_size), jnp.float32),
        jnp.zeros((tok_rows, kv_heads_here, group_size, HEAD_DIM), jnp.float32),
    )
    key_part = lax.all_gather(keys, "sp", axis=0, tiled=True)
    value_part = lax.all_gather(values, "sp", axis=0, tiled=True)
    row_count = key_part.shape[0]
    key_span = 2048
    span_count = row_count // key_span

    def scan_piece(state_in):
        key_blocks = key_part.reshape(span_count, key_span, kv_heads_here, HEAD_DIM)
        value_blocks = value_part.reshape(span_count, key_span, kv_heads_here, HEAD_DIM)
        cum_blocks = jnp.transpose(
            all_cum.reshape(span_count, key_span, kv_heads_here, group_size), (0, 2, 3, 1)
        )
        block_starts = key_span * jnp.arange(span_count, dtype=jnp.int32)
        state_out, _ = lax.scan(
            span_step, state_in, (key_blocks, value_blocks, cum_blocks, block_starts)
        )
        return state_out

    def keep_state(state_in):
        return state_in

    running_max, denominator, weighted = lax.cond(
        jnp.int32(0) <= last_query, scan_piece, keep_state, start_state
    )
    heads_out = (
        (weighted / denominator[..., None])
        .astype(jnp.bfloat16)
        .reshape(tok_rows, heads_here * HEAD_DIM)
    )
    rows_here = residual.shape[0]
    model_width = out_weight.shape[1]
    by_token = lax.all_to_all(heads_out, "tp", split_axis=0, concat_axis=1, tiled=True)
    projected = jnp.dot(
        by_token,
        lax.all_gather(out_weight, "tp", axis=0, tiled=True),
        preferred_element_type=jnp.float32,
    )
    after_exact = (
        (residual.astype(jnp.float32) + projected).astype(jnp.bfloat16).astype(jnp.float32)
    )
    normed = (
        after_exact
        * lax.rsqrt(jnp.mean(after_exact * after_exact, axis=-1, keepdims=True) + 1e-06)
        * norm_gain
    ).astype(jnp.bfloat16)
    experts_total = lax.axis_size("sp")
    top_count = routes.shape[1]
    capacity = max(2, 3 * rows_here * top_count // (2 * experts_total))
    slot_total = experts_total * capacity
    flat_routes = routes.reshape(rows_here * top_count)
    hits = (flat_routes[:, None] == jnp.arange(experts_total, dtype=jnp.int32)[None, :]).astype(
        jnp.int32
    )
    earlier = jnp.cumsum(hits, axis=0) - hits
    slot_index = (flat_routes * capacity + jnp.sum(earlier * hits, axis=1)).reshape(
        rows_here, top_count
    )
    slot_match = slot_index[:, :, None] == jnp.arange(slot_total, dtype=jnp.int32)[None, None, :]
    slot_matrix = jnp.sum(slot_match.astype(jnp.int32), axis=1).astype(jnp.bfloat16)
    outgoing = jnp.einsum(
        "rs,rd->sd", slot_matrix, normed, preferred_element_type=jnp.float32
    ).astype(jnp.bfloat16)
    arrived = lax.all_to_all(
        outgoing.reshape(experts_total, capacity, model_width),
        "sp",
        split_axis=0,
        concat_axis=0,
        tiled=True,
    )
    arrived = arrived.reshape(slot_total, model_width)
    gate_local = expert_gate[0]
    up_local = expert_up[0]
    down_local = expert_down[0]
    token_rows = lax.all_gather(arrived, "tp", axis=0, tiled=True)
    gate_val = jnp.dot(token_rows, gate_local, preferred_element_type=jnp.float32)
    up_val = jnp.dot(token_rows, up_local, preferred_element_type=jnp.float32)
    hidden = (jax.nn.silu(gate_val) * up_val).astype(jnp.bfloat16)
    summed = lax.psum_scatter(
        jnp.dot(hidden, down_local, preferred_element_type=jnp.float32)
        .astype(jnp.bfloat16)
        .astype(jnp.float32)
        .astype(jnp.bfloat16),
        "tp",
        scatter_dimension=0,
        tiled=True,
    )
    returned = lax.all_to_all(
        summed.reshape(experts_total, capacity, model_width),
        "sp",
        split_axis=0,
        concat_axis=0,
        tiled=True,
    )
    returned = returned.reshape(slot_total, model_width)
    combine_weights = jnp.sum(jnp.where(slot_match, route_weights[:, :, None], 0.0), axis=1)
    routed = jnp.dot(
        combine_weights,
        returned.astype(jnp.float32),
        precision=lax.Precision.HIGHEST,
        preferred_element_type=jnp.float32,
    )
    return (after_exact + routed).astype(jnp.bfloat16)


MOST_DIRECT = 16


def direct_shards(
    queries,
    keys,
    values,
    forget_cum,
    out_weight,
    residual,
    norm_gain,
    expert_gate,
    expert_up,
    expert_down,
    routes,
    route_weights,
):
    sp_size = lax.axis_size("sp")
    tp_size = lax.axis_size("tp")
    sp_here = lax.axis_index("sp")
    tp_here = lax.axis_index("tp")

    def over_sp(array, mask, keep=lambda place: True):
        return lax.ppermute(
            array, "sp", [(i, i ^ mask) for i in range(sp_size) if keep(i ^ mask)]
        )

    def over_tp(array, mask):
        return lax.ppermute(array, "tp", [(i, i ^ mask) for i in range(tp_size)])

    tp_bits = []
    bit = tp_size // 2
    while bit:
        tp_bits.append(bit)
        bit //= 2
    tp_masks = [0]
    for bit in tp_bits:
        tp_masks = tp_masks + [mask ^ bit for mask in tp_masks]

    def doubled(part):
        for bit in tp_bits:
            part = jnp.concatenate([part, over_tp(part, bit)], axis=0)
        return part

    def halved(part):
        for bit in reversed(tp_bits):
            half = part.shape[0] // 2
            part = (
                part[:half].astype(jnp.float32)
                + over_tp(part[half:], bit).astype(jnp.float32)
            ).astype(jnp.bfloat16)
        return part

    tok_rows = queries.shape[0]
    heads_here = forget_cum.shape[1]
    kv_heads_here = keys.shape[1] // HEAD_DIM
    group_size = heads_here // kv_heads_here
    score_scale = HEAD_DIM ** (-0.5)

    own_kv = jnp.concatenate([keys, values], axis=0)
    own_cum = forget_cum.T
    kv_parts = {0: own_kv}
    cum_parts = {0: own_cum}
    for high in range(2, sp_size, 2):
        later = lambda place, high=high: (place ^ high) < place
        kv_parts[high] = over_sp(own_kv, high, later)
        cum_parts[high] = over_sp(own_cum, high, later)
    if sp_size > 1:
        odd = lambda place: place % 2 == 1
        kv_parts[1] = over_sp(own_kv, 1, odd)
        cum_parts[1] = over_sp(own_cum, 1, odd)
    weight_parts = doubled(out_weight)
    for high in range(2, sp_size, 2):
        later = lambda place, high=high: (place ^ high) < place
        kv_parts[high + 1] = over_sp(kv_parts[high], 1, later)
        cum_parts[high + 1] = over_sp(cum_parts[high], 1, later)

    query_heads = jnp.transpose(
        queries.reshape(tok_rows, kv_heads_here, group_size, HEAD_DIM), (1, 2, 0, 3)
    )
    query_cum = own_cum.reshape(kv_heads_here, group_size, tok_rows)
    position = jnp.arange(tok_rows, dtype=jnp.int32)
    states = []
    step = min(2, sp_size)
    for first in range(0, sp_size, step):
        masks = range(first, first + step)
        k_now = jnp.concatenate([kv_parts[m][:tok_rows] for m in masks], axis=0)
        v_now = jnp.concatenate([kv_parts[m][tok_rows:] for m in masks], axis=0)
        cum_now = jnp.concatenate([cum_parts[m] for m in masks], axis=1).reshape(
            kv_heads_here, group_size, step * tok_rows
        )
        key_index = jnp.concatenate([(sp_here ^ m) * tok_rows + position for m in masks])
        query_index = sp_here * tok_rows + position
        scores = (
            jnp.einsum(
                "kgtd,ukd->kgtu",
                query_heads,
                k_now.reshape(step * tok_rows, kv_heads_here, HEAD_DIM),
                preferred_element_type=jnp.float32,
            )
            * score_scale
        )
        scores = scores + query_cum[..., None] - cum_now[:, :, None, :]
        visible = key_index[None, :] <= query_index[:, None]
        scores = jnp.where(visible[None, None], scores, -1e30)
        part_max = jnp.max(scores, axis=-1)
        weights_exp = jnp.exp(scores - part_max[..., None])
        part_sum = jnp.sum(weights_exp, axis=-1)
        part_out = jnp.einsum(
            "kgtu,ukd->kgtd",
            weights_exp.astype(jnp.bfloat16),
            v_now.reshape(step * tok_rows, kv_heads_here, HEAD_DIM),
            preferred_element_type=jnp.float32,
        )
        states.append((part_max, part_sum, part_out))
    full_max = states[0][0]
    for part_max, _, _ in states[1:]:
        full_max = jnp.maximum(full_max, part_max)
    denominator = 0.0
    weighted = 0.0
    for part_max, part_sum, part_out in states:
        rescale = jnp.exp(part_max - full_max)
        denominator = denominator + part_sum * rescale
        weighted = weighted + part_out * rescale[..., None]
    heads_out = (weighted / denominator[..., None]).astype(jnp.bfloat16)

    rows_here = residual.shape[0]
    model_width = out_weight.shape[1]
    out_rows = out_weight.shape[0]
    heads_out = jnp.transpose(
        heads_out.reshape(heads_here, tp_size, rows_here, HEAD_DIM), (1, 2, 0, 3)
    ).reshape(tp_size, rows_here, heads_here * HEAD_DIM)
    by_token = []
    for mask in tp_masks:
        block = lax.dynamic_index_in_dim(heads_out, tp_here ^ mask, 0, keepdims=False)
        by_token.append(over_tp(block, mask) if mask else block)
    projected = jnp.dot(
        jnp.concatenate(by_token, axis=1), weight_parts, preferred_element_type=jnp.float32
    )
    after_exact = (
        (residual.astype(jnp.float32) + projected).astype(jnp.bfloat16).astype(jnp.float32)
    )
    normed = (
        after_exact
        * lax.rsqrt(jnp.mean(after_exact * after_exact, axis=-1, keepdims=True) + 1e-06)
        * norm_gain
    ).astype(jnp.bfloat16)

    top_count = routes.shape[1]
    capacity = max(2, 3 * rows_here * top_count // (2 * sp_size))
    slot_total = sp_size * capacity
    flat_routes = routes.reshape(rows_here * top_count) ^ sp_here
    hits = (flat_routes[:, None] == jnp.arange(sp_size, dtype=jnp.int32)[None, :]).astype(
        jnp.int32
    )
    earlier = jnp.cumsum(hits, axis=0) - hits
    slot_index = (flat_routes * capacity + jnp.sum(earlier * hits, axis=1)).reshape(
        rows_here, top_count
    )
    slot_match = slot_index[:, :, None] == jnp.arange(slot_total, dtype=jnp.int32)[None, None, :]
    slot_matrix = jnp.sum(slot_match.astype(jnp.int32), axis=1).astype(jnp.bfloat16)
    combine_weights = jnp.sum(jnp.where(slot_match, route_weights[:, :, None], 0.0), axis=1)
    outgoing = jnp.einsum(
        "rs,rd->sd", slot_matrix, normed, preferred_element_type=jnp.float32
    ).astype(jnp.bfloat16)

    gate_local = expert_gate[0]
    up_local = expert_up[0]
    down_local = expert_down[0]
    arrived = {}
    for mask in reversed(range(sp_size)):
        block = outgoing[mask * capacity : (mask + 1) * capacity]
        arrived[mask] = over_sp(block, mask) if mask else block
    returned = {}
    for first in range(0, sp_size, step):
        masks = range(first, first + step)
        token_rows = doubled(jnp.concatenate([arrived[m] for m in masks], axis=0))
        gate_val = jnp.dot(token_rows, gate_local, preferred_element_type=jnp.float32)
        up_val = jnp.dot(token_rows, up_local, preferred_element_type=jnp.float32)
        hidden = (jax.nn.silu(gate_val) * up_val).astype(jnp.bfloat16)
        partial = jnp.dot(hidden, down_local, preferred_element_type=jnp.float32).astype(
            jnp.bfloat16
        )
        summed = halved(partial)
        for place, mask in enumerate(masks):
            block = summed[place * capacity : (place + 1) * capacity]
            returned[mask] = over_sp(block, mask) if mask else block
    back = jnp.concatenate([returned[m] for m in range(sp_size)], axis=0)
    routed = jnp.dot(
        combine_weights,
        back.astype(jnp.float32),
        precision=lax.Precision.HIGHEST,
        preferred_element_type=jnp.float32,
    )
    return (after_exact + routed).astype(jnp.bfloat16)


def power_of_two(number):
    return number & (number - 1) == 0


def solution(mesh):
    sp_size, tp_size = mesh.shape["sp"], mesh.shape["tp"]
    direct = power_of_two(sp_size) and power_of_two(tp_size) and sp_size <= MOST_DIRECT
    return jax.shard_map(
        direct_shards if direct else wide_shards,
        mesh=mesh,
        in_specs=(
            P("sp", "tp"),
            P("sp", "tp"),
            P("sp", "tp"),
            P("sp", "tp"),
            P("tp", None),
            P(("sp", "tp"), None),
            P(),
            P("sp", None, "tp"),
            P("sp", None, "tp"),
            P("sp", "tp", None),
            P(("sp", "tp"), None),
            P(("sp", "tp"), None),
        ),
        out_specs=P(("sp", "tp"), None),
        check_vma=False,
    )
```
